256 devices in a mesh: grp: 2 (over y), ep: 32 (over z, core), tp: 4 (over x).
Axes of the slice: x: 4, y: 2, z: 16, core: 2. Of those that a mesh axis runs over, the one named last changes fastest.
The devices are a block of a 4x16x16 slice.
Arguments:
- tokens: bfloat16 [16384, 2048], P(('grp', 'ep', 'tp')), parts along dimension 0, may hold values from -6 to 6
- gain_in: float32 [2048], replicated, may hold values from 0.1 to 1.9
- routes: int32 [16384, 2], P(('grp', 'ep')), parts along dimension 0, may hold values from 0 to 31, all different within a row; in each aligned block of 64 rows (0 to 63, 64 to 127, ...) at most 6 rows name the same one
- gates: float32 [16384, 2], P(('grp', 'ep')), parts along dimension 0, may hold values from 0.05 to 1
- w_gate: bfloat16 [32, 2048, 3072], P('ep', None, 'tp'), may hold values from -0.125 to 0.125
- w_up: bfloat16 [32, 2048, 3072], P('ep', None, 'tp'), may hold values from -0.125 to 0.125
- w_down: bfloat16 [32, 3072, 2048], P('ep', 'tp'), may hold values from -0.109375 to 0.109375
- gain_out: float32 [2048], P('tp'), may hold values from 0.3 to 3
Outputs:
- mixed: bfloat16 [16384, 2048], P(('grp', 'ep'), 'tp'), parts along dimension 0
The draws below stay inside these ranges and needn't reach their ends.
There are 2 independent parts, one for each index of `grp`. The reference program is written for one: setup_inputs(seed, part) draws one part's arguments, and reference() takes and returns one part's arrays. A program takes and returns all parts, laid end to end along the dimension named above; an argument that names none is the same for every part. Nothing has to cross between parts.
Inputs may be any that keep to these rules, and one draw needn't show every extreme that they name: `routes`: each row names 2 different experts; every expert is named by some row. Among the rows of one device (aligned blocks of 64 rows) no expert is named more than 6 times, and in every draw some expert is named exactly 6 times in some such block.
All inputs are finite; a program needn't handle non-finite values.
Results may differ from the reference program's by a relative error of at most 0.012.
Values may be sent and summed in bfloat16 or wider, within the bound.
No kernel may reach another device: no remote copies, remote signals or barrier semaphores. Data moves between devices by JAX's collectives and lax.ppermute only.
A program may use at most 64 MiB of HBM per device.

```python
import math
import jax
import jax.numpy as jnp
import numpy as np
from jax import lax

D = 2048
FF = 3072
TOPK = 2
TOK_DEV = 64
EXPERTS = 32
CAP = 6
FF_DEV = 768
TOKENS = 8192
N_EP = 32
N_TP = 4


def level_of(own_key, extent, split, smallest, top_value):
    level = 1.0
    for dim, blocks in split:
        heights = jax.random.uniform(jax.random.fold_in(jax.random.fold_in(own_key, 6), dim), (blocks,), jnp.float32, smallest / len(split), top_value / len(split))
        level = level * jnp.repeat(jnp.exp(heights), extent[dim] // blocks).reshape((-1,) + (1,) * (len(extent) - 1 - dim))
    return level


def deal_out(rng, own, number, rows, amount, top, reach, lean):
    sequence = jax.random.permutation(rng, amount)
    crowded, common = load_shares(amount, rows * top, reach, lean, True), load_shares(amount, rows * top, reach, lean, False)
    places = jnp.arange(amount)

    def named(tallies, turn):
        used = int((tallies > 0).sum())
        fixed = max(1, used // 4)
        passed = fixed + (places - fixed + turn * (used - fixed)) % max(1, amount - fixed)
        return jnp.zeros((amount,), jnp.int32).at[sequence[jnp.where(places < fixed, places, passed)]].set(jnp.asarray(tallies, jnp.int32))

    tallies = jnp.where(number % 4 == 0, named(crowded, number // 4), named(common, number - number // 4 - 1))
    mixed = jax.random.permutation(jax.random.fold_in(own, 3), amount)
    donor, taker = mixed[0:amount // 2 * 2:2], mixed[1:amount // 2 * 2:2]
    slack = jnp.minimum(tallies[donor] - 1, reach - tallies[taker]) // 2
    slack = jnp.where((donor == sequence[0]) | (taker == sequence[0]) | (tallies[taker] == 0), 0, jnp.maximum(slack, 0))
    passed = jax.random.randint(jax.random.fold_in(own, 4), (amount // 2,), 0, 1 << 20) % (slack + 1)
    tallies = tallies.at[donor].add(-passed).at[taker].add(passed)
    members = jnp.searchsorted(jnp.cumsum(tallies), jnp.arange(rows * top), side="right").astype(jnp.int32)
    listing = members.reshape(top, rows).T
    listing = listing[jax.random.permutation(jax.random.fold_in(own, 1), rows)]
    turn = jax.random.randint(jax.random.fold_in(own, 2), (rows, 1), 0, top)
    return jnp.take_along_axis(listing, (jnp.arange(top)[None, :] + turn) % top, axis=1)


def load_shares(number_of, total, reach, slope, full):
    portions = [(1 << 20) // math.isqrt(standing ** slope) + 1 for standing in range(1, number_of + 1)]
    largest = reach if full else min(reach, max(-(-total // number_of), total * portions[0] // sum(portions)))
    least = 1 if total - largest >= number_of - 1 else 0
    holding, spare = [largest] + [least] * (number_of - 1), total - largest - least * (number_of - 1)
    while spare > 0:
        movable = [i for i in range(1, number_of) if holding[i] < largest] or [i for i in range(1, number_of) if holding[i] < reach]
        pool, remaining = sum([portions[i] for i in movable]), spare
        for i in movable:
            extra = min(reach - holding[i], max(1, remaining * portions[i] // pool), spare)
            holding[i] = holding[i] + extra
            spare = spare - extra
    return np.array(holding)


def bell_draw(own_key, shape, scale, reach, pieces=(), held_as=jnp.bfloat16):
    values = jax.random.normal(own_key, shape, jnp.float32) * scale
    if len(pieces) > 0:
        values = level_of(own_key, shape, pieces, -0.22, 0.18) * values
    return jnp.clip(values, min=-reach, max=reach).astype(held_as)


def setup_inputs(seed: int = 0, part: int = 0) -> dict:
    streams_of = jax.random.split(jax.random.key(seed), 9)
    part_keys = jax.random.split(jax.random.fold_in(streams_of[8], part), 9)
    tokens = bell_draw(part_keys[0], (TOKENS, D), 1.0, 6.0, ((0, 128),))
    gain_in = jnp.clip(1.0 + 0.18 * jax.random.normal(streams_of[1], (D,), jnp.float32), 0.1, 1.9)
    routes_keys = jax.random.split(jax.random.fold_in(part_keys[2], 1), TOKENS // TOK_DEV)
    routes_turns = jax.random.permutation(jax.random.fold_in(part_keys[2], 3), TOKENS // TOK_DEV)
    routes = jax.vmap(lambda own, number: deal_out(jax.random.fold_in(part_keys[2], 2), own, number, TOK_DEV, EXPERTS, TOPK, CAP, 2))(routes_keys, routes_turns).reshape((TOKENS, TOPK))
    gates = jnp.clip(0.05 + 0.95 * jax.random.uniform(part_keys[3], (TOKENS, TOPK), jnp.float32) ** level_of(part_keys[3], (TOKENS, TOPK), ((0, 32),), -0.2, 0.2), 0.05, 1.0)
    w_gate = bell_draw(streams_of[4], (EXPERTS, D, FF), D ** -0.5, 0.125, ((0, 32), (2, 4)))
    w_up = bell_draw(streams_of[5], (EXPERTS, D, FF), D ** -0.5, 0.125, ((0, 32), (2, 4)))
    w_down = bell_draw(streams_of[6], (EXPERTS, FF, D), FF ** -0.5, 0.109375, ((0, 32), (1, 4)))
    gain_out = jnp.clip(jnp.exp(math.log(3.0) - 2.3025851 * jax.random.uniform(streams_of[7], (D,), jnp.float32) ** level_of(streams_of[7], (D,), ((0, 4),), -0.2, 0.2)), 0.3, 3.0)
    return {"tokens": tokens, "gain_in": gain_in, "routes": routes, "gates": gates, "w_gate": w_gate, "w_up": w_up, "w_down": w_down, "gain_out": gain_out}


EPS = 1e-06

def reference(tokens, gain_in, routes, gates, w_gate, w_up, w_down, gain_out):
    values = tokens.astype(jnp.float32)
    normed = (values * lax.rsqrt(lax.optimization_barrier(jnp.mean(values * values, axis=-1, keepdims=True)) + EPS) * gain_in).astype(jnp.bfloat16)
    most = N_EP * N_TP * CAP
    blocks = FF // FF_DEV

    def one_expert(total, items):
        expert, gate_w, up_w, down_w = items
        hit = routes == expert
        chosen = jnp.any(hit, axis=1)
        index = jnp.nonzero(chosen, size=most, fill_value=0)[0].astype(jnp.int32)
        count = jnp.sum(chosen.astype(jnp.int32))
        live = (jnp.arange(most, dtype=jnp.int32) < count).astype(jnp.float32)
        rows = normed[index]
        gate = jnp.dot(rows, gate_w, preferred_element_type=jnp.float32)
        up = jnp.dot(rows, up_w, preferred_element_type=jnp.float32)
        hidden = (jax.nn.silu(gate) * up).astype(jnp.bfloat16)
        parts = jnp.einsum('rbf,bfd->brd', hidden.reshape(most, blocks, FF_DEV).astype(jnp.float32), down_w.reshape(blocks, FF_DEV, D).astype(jnp.float32))
        rounded = lax.optimization_barrier(parts.astype(jnp.bfloat16))
        summed = lax.optimization_barrier(jnp.sum(rounded.astype(jnp.float32), axis=0))
        result = lax.optimization_barrier(summed.astype(jnp.bfloat16)).astype(jnp.float32)
        weight = lax.optimization_barrier(jnp.sum(jnp.where(hit, gates, jnp.float32(0.0)), axis=1))[index] * live
        total = total.at[index].add(weight[:, None] * result)
        return (total, None)
    start = jnp.zeros((TOKENS, D), jnp.float32)
    combined, unused = lax.scan(one_expert, start, (jnp.arange(EXPERTS, dtype=jnp.int32), w_gate, w_up, w_down))
    scale = lax.rsqrt(lax.optimization_barrier(jnp.mean(combined * combined, axis=-1, keepdims=True)) + EPS)
    return (combined * scale * gain_out).astype(jnp.bfloat16)
```

```python
import jax
import jax.numpy as jnp
from jax import lax
from jax.sharding import PartitionSpec as P

EPS = 1e-06
CHUNKS = 2


def rotate(value, axis, step):
    size = lax.axis_size(axis)
    return lax.ppermute(value, axis, [(i, (i + step) % size) for i in range(size)])


def partner(value):
    return lax.ppermute(value, "ep", [(i, i ^ 1) for i in range(lax.axis_size("ep"))])


def exchange(value):
    size = lax.axis_size("ep")
    same = [list(range(core, size, 2)) for core in range(2)]
    return lax.all_to_all(value, "ep", 0, 0, tiled=True, axis_index_groups=same)


def slots_of(routes):
    flat = routes.reshape(-1)
    count = flat.shape[0]
    order = jnp.arange(count, dtype=jnp.int32)
    earlier = (flat[None, :] == flat[:, None]) & (order[None, :] < order[:, None])
    return jnp.sum(earlier.astype(jnp.int32), axis=1).reshape(routes.shape)


def gather_blocks(own):
    half = own.shape[0] // 2
    before = rotate(own, "tp", 1)
    after = rotate(own, "tp", -1)
    far = jnp.concatenate(
        [rotate(before[:half], "tp", 1), rotate(after[half:], "tp", -1)], axis=0
    )
    return [own, after, far, before]


def scatter_blocks(blocks):
    own, up, far, down = blocks
    half = own.shape[0] // 2
    wide = jnp.float32
    from_before = rotate(far[:half], "tp", 1)
    from_after = rotate(far[half:], "tp", -1)
    up = jnp.concatenate(
        [(up[:half].astype(wide) + from_before.astype(wide)).astype(up.dtype), up[half:]], axis=0
    )
    down = jnp.concatenate(
        [down[:half], (down[half:].astype(wide) + from_after.astype(wide)).astype(up.dtype)],
        axis=0,
    )
    return own.astype(wide) + rotate(up, "tp", 1).astype(wide) + rotate(down, "tp", -1).astype(wide)


def place(key_rows, key_columns):
    return jnp.any(key_rows == key_columns, axis=0)


def local(tokens, gain_in, routes, gates, w_gate, w_up, w_down, gain_out):
    count, width = tokens.shape
    choose = routes.shape[1]
    experts = lax.axis_size("ep")
    groups = lax.axis_size("tp")
    chips = experts // 2
    capacity = (3 * count * choose + 2 * experts - 1) // (2 * experts)
    part = capacity // CHUNKS
    lanes = width // groups
    hidden_width = w_gate.shape[2]
    narrow = jnp.bfloat16
    me = lax.axis_index("tp")
    core = lax.axis_index("ep") % 2

    own_routes = lax.dynamic_slice_in_dim(routes, me * count, count, 0)
    own_gates = lax.dynamic_slice_in_dim(gates, me * count, count, 0)
    both_tokens = jnp.concatenate([tokens, partner(tokens)], axis=0)
    other_routes = partner(own_routes)
    own_places = own_routes * capacity + slots_of(own_routes)
    other_places = other_routes * capacity + slots_of(other_routes)
    span = experts * capacity

    values = both_tokens.astype(jnp.float32)
    normed = (
        values * lax.rsqrt(jnp.mean(values * values, axis=-1, keepdims=True) + EPS) * gain_in
    ).astype(narrow)
    stacked = jnp.concatenate(
        [normed[:, q * lanes : (q + 1) * lanes] for q in range(groups)], axis=0
    )
    quarter = jnp.arange(groups, dtype=jnp.int32)
    sent_keys = jnp.stack([own_places, other_places + span]).transpose(2, 0, 1)
    sent_keys = sent_keys[:, None] + (quarter * 2 * span)[None, :, None, None]
    sent_keys = sent_keys.reshape(choose, 1, groups * 2 * count)

    rows = chips * 2 * part * groups
    row = jnp.arange(rows, dtype=jnp.int32)
    row_quarter = row % groups
    row_slot = (row // groups) % part
    row_side = (row // (groups * part)) % 2
    row_chip = row // (groups * part * 2)

    gains = [gain_out] + [rotate(gain_out[None], "tp", -step)[0] for step in range(1, groups)]

    block = chips * 2 * part
    line = jnp.arange(block, dtype=jnp.int32)
    line_slot = line % part
    line_chip = (line // part) % chips
    line_side = line // (part * chips)
    line_row = ((line_chip * 2 + line_side) * part + line_slot) * groups

    arrived = []
    for k in range(CHUNKS):
        key = (row_quarter * 2 + row_side) * span + (
            (2 * row_chip + core) * capacity + part * k + row_slot
        )
        select = place(key[None, :, None], sent_keys).astype(narrow)
        outgoing = jnp.dot(select, stacked, preferred_element_type=jnp.float32).astype(narrow)
        arrived.append(exchange(outgoing.reshape(chips, -1, lanes)).reshape(rows, lanes))

    returned = []
    for k in range(CHUNKS):
        own = jnp.concatenate(
            [
                jnp.dot(
                    (line_row[:, None] + q == row[None, :]).astype(narrow),
                    arrived[k],
                    preferred_element_type=jnp.float32,
                ).astype(narrow)
                for q in range(groups)
            ],
            axis=1,
        )
        flat = jnp.concatenate(gather_blocks(own), axis=0)
        gate = jnp.dot(flat, w_gate[0], preferred_element_type=jnp.float32)
        up = jnp.dot(flat, w_up[0], preferred_element_type=jnp.float32)
        hidden = (jax.nn.silu(gate) * up).astype(narrow)
        down = jnp.dot(hidden, w_down[0], preferred_element_type=jnp.float32).astype(narrow)
        summed = scatter_blocks([down[i * block : (i + 1) * block] for i in range(groups)])
        summed = summed.astype(narrow)
        half = block // 2
        mine = jnp.concatenate([summed[:half], partner(summed[half:])], axis=0)
        tall = jnp.concatenate(
            [mine[:, q * lanes : (q + 1) * lanes] for q in range(groups)], axis=0
        )
        back = (
            (row_quarter[:, None] * block + (row_side * chips + row_chip)[:, None] * part)
            + row_slot[:, None]
            == jnp.arange(groups * block, dtype=jnp.int32)[None, :]
        ).astype(narrow)
        leaving = jnp.dot(back, tall, preferred_element_type=jnp.float32).astype(narrow)
        returned.append(exchange(leaving.reshape(chips, -1, lanes)).reshape(rows, lanes))

    combined = 0.0
    wanted = (((me + quarter) % groups) * span)[None, :, None] + own_places.T[:, None, :]
    wanted = wanted.reshape(choose, groups * count, 1)
    weights = jnp.broadcast_to(own_gates.T[:, None, :], (choose, groups, count))
    weights = weights.reshape(choose, groups * count, 1)
    for k in range(CHUNKS):
        key = row_quarter * span + (
            (2 * row_chip + (core ^ row_side)) * capacity + part * k + row_slot
        )
        combine = jnp.sum(jnp.where(wanted == key[None, None, :], weights, jnp.float32(0.0)), axis=0)
        high = lax.reduce_precision(combine, 8, 7)
        combined = combined + jnp.dot(
            high.astype(narrow), returned[k], preferred_element_type=jnp.float32
        )
        combined = combined + jnp.dot(
            (combine - high).astype(narrow), returned[k], preferred_element_type=jnp.float32
        )
    combined = combined.reshape(groups, count, lanes)
    squares = jnp.sum(combined * combined, axis=(0, 2))
    scale = lax.rsqrt(squares / width + EPS)
    final = [
        (combined[step] * scale[:, None] * gains[step]).astype(narrow) for step in range(groups)
    ]
    final = [final[0]] + [rotate(final[step], "tp", step) for step in range(1, groups)]
    out = []
    for j in range(groups):
        piece = final[0]
        for step in range(1, groups):
            piece = jnp.where((me - step) % groups == j, final[step], piece)
        out.append(piece)
    return jnp.concatenate(out, axis=0)


def solution(mesh):
    in_specs = (
        P(("grp", "ep", "tp"), None),
        P(),
        P(("grp", "ep"), None),
        P(("grp", "ep"), None),
        P("ep", None, "tp"),
        P("ep", None, "tp"),
        P("ep", "tp", None),
        P("tp"),
    )
    out_specs = P(("grp", "ep"), "tp")
    return jax.shard_map(local, mesh=mesh, in_specs=in_specs, out_specs=out_specs, check_vma=False)
```

```python
import functools

import jax
import jax.numpy as jnp
from jax import lax
from jax.experimental import pallas as pl
from jax.experimental.pallas import tpu as pltpu
from jax.sharding import PartitionSpec as P


EPS = 1e-06
CHUNKS = 2
TILE = 256
NARROW = jnp.bfloat16
WIDE = jnp.float32
VMEM_LIMIT = 48 * 1024 * 1024


def rotate(value, axis, step):
    size = lax.axis_size(axis)
    return lax.ppermute(value, axis, [(i, (i + step) % size) for i in range(size)])


def partner(value):
    return lax.ppermute(value, "ep", [(i, i ^ 1) for i in range(lax.axis_size("ep"))])


def exchange(value):
    size = lax.axis_size("ep")
    same = [list(range(core, size, 2)) for core in range(2)]
    return lax.all_to_all(value, "ep", 0, 0, tiled=True, axis_index_groups=same)


def dot(a, b):
    return jnp.dot(a, b, preferred_element_type=WIDE)


def one_hot(matches):
    return jnp.where(matches, 1.0, 0.0).astype(NARROW)


def places(own, other, capacity, span):
    both = jnp.concatenate([own * capacity, other * capacity + span], axis=0)
    column = jnp.concatenate([both[:, c : c + 1] for c in range(both.shape[1])], axis=0)
    total = column.shape[0]
    i = lax.broadcasted_iota(jnp.int32, (total, total), 0)
    j = lax.broadcasted_iota(jnp.int32, (total, total), 1)
    row = jnp.sum(jnp.where(i == j, column, 0), axis=0, keepdims=True)
    same = column == row
    row_slot = jnp.sum(jnp.where(same & (i < j), 1, 0), axis=0, keepdims=True)
    column_slot = jnp.sum(jnp.where(same & (j < i), 1, 0), axis=1, keepdims=True)
    return column + column_slot, row + row_slot


def pack_kernel(own, other, gain, own_routes, other_routes, row_key, *outs, capacity, span, groups):
    values = jnp.concatenate([own[...], other[...]], axis=0).astype(WIDE)
    scale = lax.rsqrt(jnp.mean(values * values, axis=-1, keepdims=True) + EPS)
    normed = (values * scale * gain[...]).astype(NARROW)
    _, row = places(own_routes[...], other_routes[...], capacity, span)
    rows = values.shape[0]
    lanes = values.shape[1] // groups
    for k, out in enumerate(outs):
        key = row_key[...] + k * (capacity // len(outs))
        total = None
        for q in range(groups):
            hit = key == row[:, :rows] + q * 2 * span
            for c in range(1, row.shape[1] // rows):
                hit = hit | (key == row[:, c * rows : (c + 1) * rows] + q * 2 * span)
            piece = dot(one_hot(hit), normed[:, q * lanes : (q + 1) * lanes])
            total = piece if total is None else total + piece
        out[...] = total.astype(NARROW)


def spread_kernel(arrived, line_row, out, *, groups):
    lanes = arrived.shape[1]
    column = lax.broadcasted_iota(jnp.int32, (line_row.shape[0], arrived.shape[0]), 1)
    for q in range(groups):
        pick = one_hot(line_row[...] + q == column)
        out[:, q * lanes : (q + 1) * lanes] = dot(pick, arrived[...]).astype(NARROW)


def expert_kernel(*refs):
    sources, (wg, wu, wd), sinks, (flat, acc) = refs[:5], refs[5:8], refs[8:13], refs[13:]
    step = pl.program_id(0)

    @pl.when(step == 0)
    def _():
        at = 0
        for source in sources:
            flat[at : at + source.shape[0], :] = source[...]
            at += source.shape[0]

    gate = dot(flat[...], wg[0])
    up = dot(flat[...], wu[0])
    hidden = (gate / (1.0 + jnp.exp(-gate)) * up).astype(NARROW)
    down = dot(hidden, wd[0])

    @pl.when(step == 0)
    def _():
        acc[...] = down

    @pl.when(step > 0)
    def _():
        acc[...] += down

    @pl.when(step == pl.num_programs(0) - 1)
    def _():
        at = 0
        for sink in sinks:
            sink[...] = acc[at : at + sink.shape[0], :].astype(sink.dtype)
            at += sink.shape[0]


def leave_kernel(kept, got, back, out, *, groups):
    both = jnp.concatenate([kept[...], got[...]], axis=0)
    lanes = both.shape[1] // groups
    column = lax.broadcasted_iota(jnp.int32, (out.shape[0], both.shape[0]), 1)
    total = None
    for q in range(groups):
        pick = one_hot(back[...] == column + q * both.shape[0])
        piece = dot(pick, both[:, q * lanes : (q + 1) * lanes])
        total = piece if total is None else total + piece
    out[...] = total.astype(NARROW)


def finish_kernel(*refs, capacity, span, groups):
    returned = refs[:CHUNKS]
    own_routes, other_routes, gates, column_key, quarters = refs[CHUNKS : CHUNKS + 5]
    gains = refs[CHUNKS + 5 : CHUNKS + 5 + groups]
    outs = refs[CHUNKS + 5 + groups :]
    column, _ = places(own_routes[...], other_routes[...], capacity, span)
    count, choose = gates.shape
    width = groups * returned[0].shape[1]
    total = None
    for k in range(CHUNKS):
        key = column_key[...] + k * (capacity // CHUNKS)
        blocks = []
        for step in range(groups):
            weight = 0.0
            for c in range(choose):
                place = column[2 * c * count : (2 * c + 1) * count, :] + quarters[step]
                weight = weight + jnp.where(place == key, gates[:, c : c + 1], 0.0)
            blocks.append(weight)
        weight = jnp.concatenate(blocks, axis=0)
        high = weight.astype(NARROW)
        low = (weight - high.astype(WIDE)).astype(NARROW)
        piece = dot(high, returned[k][...]) + dot(low, returned[k][...])
        total = piece if total is None else total + piece
    squares = 0.0
    for step in range(groups):
        block = total[step * count : (step + 1) * count, :]
        squares = squares + jnp.sum(block * block, axis=1, keepdims=True)
    scale = lax.rsqrt(squares / width + EPS)
    for step in range(groups):
        block = total[step * count : (step + 1) * count, :]
        outs[step][...] = (block * scale * gains[step][...]).astype(NARROW)


def whole(spec):
    return jax.ShapeDtypeStruct(spec[0], spec[1])


def call(kernel, outs, *args, flops=0, moved=0, smem=(), **kwargs):
    return pl.pallas_call(
        functools.partial(kernel, **kwargs),
        out_shape=[whole(o) for o in outs],
        in_specs=[
            pl.BlockSpec(memory_space=pltpu.SMEM if i in smem else pltpu.VMEM)
            for i in range(len(args))
        ],
        out_specs=[pl.BlockSpec(memory_space=pltpu.VMEM) for _ in outs],
        cost_estimate=pl.CostEstimate(flops=flops, bytes_accessed=moved, transcendentals=0),
        compiler_params=pltpu.CompilerParams(vmem_limit_bytes=VMEM_LIMIT),
    )(*args)


def expert(sources, w_gate, w_up, w_down):
    _, width = sources[0].shape
    hidden = w_gate.shape[2]
    total = sum(s.shape[0] for s in sources)
    dtypes = [WIDE] + [NARROW] * (len(sources) - 1)
    fixed = lambda s: pl.BlockSpec(s.shape, lambda j: (0, 0))
    return pl.pallas_call(
        expert_kernel,
        grid=(hidden // TILE,),
        out_shape=[jax.ShapeDtypeStruct(s.shape, d) for s, d in zip(sources, dtypes)],
        in_specs=[fixed(s) for s in sources]
        + [
            pl.BlockSpec((1, width, TILE), lambda j: (0, 0, j)),
            pl.BlockSpec((1, width, TILE), lambda j: (0, 0, j)),
            pl.BlockSpec((1, TILE, width), lambda j: (0, j, 0)),
        ],
        out_specs=[fixed(s) for s in sources],
        scratch_shapes=[pltpu.VMEM((total, width), NARROW), pltpu.VMEM((total, width), WIDE)],
        cost_estimate=pl.CostEstimate(
            flops=6 * total * width * hidden,
            bytes_accessed=6 * width * hidden + 8 * total * width,
            transcendentals=total * hidden,
        ),
        compiler_params=pltpu.CompilerParams(
            dimension_semantics=("arbitrary",), vmem_limit_bytes=VMEM_LIMIT
        ),
    )(*sources, w_gate, w_up, w_down)


def gather_blocks(own):
    half = own.shape[0] // 2
    before = rotate(own, "tp", 1)
    after = rotate(own, "tp", -1)
    return [
        own,
        after,
        rotate(before[:half], "tp", 1),
        rotate(after[half:], "tp", -1),
        before,
    ]


def scatter_blocks(blocks):
    own, up, far_low, far_high, down = blocks
    half = own.shape[0] // 2
    from_before = rotate(far_low, "tp", 1)
    from_after = rotate(far_high, "tp", -1)
    up = jnp.concatenate(
        [(up[:half].astype(WIDE) + from_before.astype(WIDE)).astype(NARROW), up[half:]], axis=0
    )
    down = jnp.concatenate(
        [down[:half], (down[half:].astype(WIDE) + from_after.astype(WIDE)).astype(NARROW)], axis=0
    )
    up = rotate(up, "tp", 1).astype(WIDE)
    down = rotate(down, "tp", -1).astype(WIDE)
    return [
        (own[p] + up[p] + down[p]).astype(NARROW) for p in (slice(0, half), slice(half, None))
    ]


def local(tokens, gain_in, routes, gates, w_gate, w_up, w_down, gain_out):
    count, width = tokens.shape
    choose = routes.shape[1]
    experts = lax.axis_size("ep")
    groups = lax.axis_size("tp")
    chips = experts // 2
    capacity = (3 * count * choose + 2 * experts - 1) // (2 * experts)
    span = experts * capacity
    part = capacity // CHUNKS
    lanes = width // groups
    rows = chips * 2 * part * groups
    block = chips * 2 * part
    me = lax.axis_index("tp")
    core = lax.axis_index("ep") % 2

    own_routes = lax.dynamic_slice_in_dim(routes, me * count, count, 0)
    own_gates = lax.dynamic_slice_in_dim(gates, me * count, count, 0)
    other_routes = partner(own_routes)
    other_tokens = partner(tokens)

    row = jnp.arange(rows, dtype=jnp.int32)[:, None]
    quarter = row % groups
    slot = (row // groups) % part
    side = (row // (groups * part)) % 2
    chip = row // (groups * part * 2)
    row_key = (quarter * 2 + side) * span + (2 * chip + core) * capacity + slot
    column_key = (quarter * span + (2 * chip + (core ^ side)) * capacity + slot).reshape(1, rows)
    back = quarter * block + (side * chips + chip) * part + slot
    line = jnp.arange(block, dtype=jnp.int32)[:, None]
    line_row = ((line // part) % chips * 2 + line // (part * chips)) * part + line % part
    line_row = line_row * groups
    quarters = (me + jnp.arange(groups, dtype=jnp.int32)) % groups * span

    outgoing = call(
        pack_kernel,
        [((rows, lanes), NARROW)] * CHUNKS,
        tokens,
        other_tokens,
        gain_in[None],
        own_routes,
        other_routes,
        row_key,
        capacity=capacity,
        span=span,
        groups=groups,
        flops=2 * CHUNKS * rows * 2 * count * width,
        moved=4 * count * width,
    )
    arrived = []
    for k in range(CHUNKS):
        arrived.append(exchange(outgoing[k].reshape(chips, -1, lanes)).reshape(rows, lanes))
    gains = [gain_out[None]]
    gains += [rotate(gain_out[None], "tp", -step) for step in range(1, groups)]

    returned = []
    for k in range(CHUNKS):
        (own,) = call(
            spread_kernel,
            [((block, width), NARROW)],
            arrived[k],
            line_row,
            groups=groups,
            flops=2 * block * rows * width,
            moved=4 * block * width,
        )
        sources = gather_blocks(own)
        parts = expert(sources, w_gate, w_up, w_down)
        kept, sent = scatter_blocks(parts)
        got = partner(sent)
        (leaving,) = call(
            leave_kernel,
            [((rows, lanes), NARROW)],
            kept,
            got,
            back,
            groups=groups,
            flops=2 * rows * block * width,
            moved=4 * block * width,
        )
        returned.append(exchange(leaving.reshape(chips, -1, lanes)).reshape(rows, lanes))

    final = call(
        finish_kernel,
        [((count, lanes), NARROW)] * groups,
        *returned,
        own_routes,
        other_routes,
        own_gates,
        column_key,
        quarters,
        *gains,
        smem=(CHUNKS + 4,),
        capacity=capacity,
        span=span,
        groups=groups,
        flops=4 * CHUNKS * rows * groups * count * lanes,
        moved=4 * rows * lanes,
    )
    final = [final[0]] + [rotate(final[step], "tp", step) for step in range(1, groups)]
    out = []
    for j in range(groups):
        piece = final[0]
        for step in range(1, groups):
            piece = jnp.where((me - step) % groups == j, final[step], piece)
        out.append(piece)
    return jnp.concatenate(out, axis=0)


def solution(mesh):
    in_specs = (
        P(("grp", "ep", "tp"), None),
        P(),
        P(("grp", "ep"), None),
        P(("grp", "ep"), None),
        P("ep", None, "tp"),
        P("ep", None, "tp"),
        P("ep", "tp", None),
        P("tp"),
    )
    out_specs = P(("grp", "ep"), "tp")
    return jax.shard_map(local, mesh=mesh, in_specs=in_specs, out_specs=out_specs, check_vma=False)
```

```python
import functools

import jax
import jax.numpy as jnp
from jax import lax
from jax.experimental import pallas as pl
from jax.experimental.pallas import tpu as pltpu
from jax.sharding import PartitionSpec as P


EPS = 1e-06
CHUNKS = 2
TILE = 256
OUT_TILE = 512
NARROW = jnp.bfloat16
WIDE = jnp.float32
VMEM_LIMIT = 48 * 1024 * 1024


def rotate(value, axis, step):
    size = lax.axis_size(axis)
    return lax.ppermute(value, axis, [(i, (i + step) % size) for i in range(size)])


def partner(value):
    return lax.ppermute(value, "ep", [(i, i ^ 1) for i in range(lax.axis_size("ep"))])


def exchange(value):
    size = lax.axis_size("ep")
    same = [list(range(core, size, 2)) for core in range(2)]
    return lax.all_to_all(value, "ep", 0, 0, tiled=True, axis_index_groups=same)


def dot(a, b):
    return jnp.dot(a, b, preferred_element_type=WIDE)


def one_hot(matches):
    return jnp.where(matches, 1.0, 0.0).astype(NARROW)


def places(own, other, capacity, span):
    both = jnp.concatenate([own * capacity, other * capacity + span], axis=0)
    column = jnp.concatenate([both[:, c : c + 1] for c in range(both.shape[1])], axis=0)
    total = column.shape[0]
    i = lax.broadcasted_iota(jnp.int32, (total, total), 0)
    j = lax.broadcasted_iota(jnp.int32, (total, total), 1)
    row = jnp.sum(jnp.where(i == j, column, 0), axis=0, keepdims=True)
    same = column == row
    row_slot = jnp.sum(jnp.where(same & (i < j), 1, 0), axis=0, keepdims=True)
    column_slot = jnp.sum(jnp.where(same & (j < i), 1, 0), axis=1, keepdims=True)
    return column + column_slot, row + row_slot


def pack_kernel(own, other, gain, own_routes, other_routes, row_key, *outs, capacity, span, groups):
    values = jnp.concatenate([own[...], other[...]], axis=0).astype(WIDE)
    scale = lax.rsqrt(jnp.mean(values * values, axis=-1, keepdims=True) + EPS)
    normed = (values * scale * gain[...]).astype(NARROW)
    _, row = places(own_routes[...], other_routes[...], capacity, span)
    rows = values.shape[0]
    lanes = values.shape[1] // groups
    for k, out in enumerate(outs):
        key = row_key[...] + k * (capacity // len(outs))
        total = None
        for q in range(groups):
            hit = key == row[:, :rows] + q * 2 * span
            for c in range(1, row.shape[1] // rows):
                hit = hit | (key == row[:, c * rows : (c + 1) * rows] + q * 2 * span)
            piece = dot(one_hot(hit), normed[:, q * lanes : (q + 1) * lanes])
            total = piece if total is None else total + piece
        out[...] = total.astype(NARROW)


def spread_kernel(arrived, line_row, out, *, groups):
    lanes = arrived.shape[1]
    column = lax.broadcasted_iota(jnp.int32, (line_row.shape[0], arrived.shape[0]), 1)
    for q in range(groups):
        pick = one_hot(line_row[...] + q == column)
        out[:, q * lanes : (q + 1) * lanes] = dot(pick, arrived[...]).astype(NARROW)


def expert_kernel(*refs):
    sources, weights, sinks = refs[:5], refs[5:8], refs[8:13]
    flat, hidden, wg, wu, wd, sems = refs[13:]
    steps = hidden.shape[1] // TILE
    loads = []
    for j in range(steps):
        part = pl.ds(j * TILE, TILE)
        for n, (source, kept) in enumerate(zip(weights, (wg, wu))):
            loads.append(
                pltpu.make_async_copy(source.at[0, :, part], kept.at[j], sems.at[2 * j + n])
            )
    loads.append(pltpu.make_async_copy(weights[2].at[0], wd, sems.at[2 * steps]))
    for load in loads:
        load.start()
    at = 0
    for source in sources:
        flat[at : at + source.shape[0], :] = source[...]
        at += source.shape[0]
    for j in range(steps):
        loads[2 * j].wait()
        loads[2 * j + 1].wait()
        gate = dot(flat[...], wg[j])
        up = dot(flat[...], wu[j])
        hidden[:, j * TILE : (j + 1) * TILE] = (gate / (1.0 + jnp.exp(-gate)) * up).astype(NARROW)
    loads[2 * steps].wait()
    for j in range(0, flat.shape[1], OUT_TILE):
        down = dot(hidden[...], wd[:, j : j + OUT_TILE])
        at = 0
        for sink in sinks:
            sink[:, j : j + OUT_TILE] = down[at : at + sink.shape[0], :].astype(sink.dtype)
            at += sink.shape[0]


def leave_kernel(kept, got, back, out, *, groups):
    both = jnp.concatenate([kept[...], got[...]], axis=0)
    lanes = both.shape[1] // groups
    column = lax.broadcasted_iota(jnp.int32, (out.shape[0], both.shape[0]), 1)
    total = None
    for q in range(groups):
        pick = one_hot(back[...] == column + q * both.shape[0])
        piece = dot(pick, both[:, q * lanes : (q + 1) * lanes])
        total = piece if total is None else total + piece
    out[...] = total.astype(NARROW)


def finish_kernel(*refs, capacity, span, groups):
    returned = refs[:CHUNKS]
    own_routes, other_routes, gates, column_key, quarters = refs[CHUNKS : CHUNKS + 5]
    gains = refs[CHUNKS + 5 : CHUNKS + 5 + groups]
    outs = refs[CHUNKS + 5 + groups :]
    column, _ = places(own_routes[...], other_routes[...], capacity, span)
    count, choose = gates.shape
    width = groups * returned[0].shape[1]
    total = None
    for k in range(CHUNKS):
        key = column_key[...] + k * (capacity // CHUNKS)
        blocks = []
        for step in range(groups):
            weight = 0.0
            for c in range(choose):
                place = column[2 * c * count : (2 * c + 1) * count, :] + quarters[step]
                weight = weight + jnp.where(place == key, gates[:, c : c + 1], 0.0)
            blocks.append(weight)
        weight = jnp.concatenate(blocks, axis=0)
        high = weight.astype(NARROW)
        low = (weight - high.astype(WIDE)).astype(NARROW)
        piece = dot(high, returned[k][...]) + dot(low, returned[k][...])
        total = piece if total is None else total + piece
    squares = 0.0
    for step in range(groups):
        block = total[step * count : (step + 1) * count, :]
        squares = squares + jnp.sum(block * block, axis=1, keepdims=True)
    scale = lax.rsqrt(squares / width + EPS)
    for step in range(groups):
        block = total[step * count : (step + 1) * count, :]
        outs[step][...] = (block * scale * gains[step][...]).astype(NARROW)


def whole(spec):
    return jax.ShapeDtypeStruct(spec[0], spec[1])


def call(kernel, outs, *args, flops=0, moved=0, smem=(), **kwargs):
    return pl.pallas_call(
        functools.partial(kernel, **kwargs),
        out_shape=[whole(o) for o in outs],
        in_specs=[
            pl.BlockSpec(memory_space=pltpu.SMEM if i in smem else pltpu.VMEM)
            for i in range(len(args))
        ],
        out_specs=[pl.BlockSpec(memory_space=pltpu.VMEM) for _ in outs],
        cost_estimate=pl.CostEstimate(flops=flops, bytes_accessed=moved, transcendentals=0),
        compiler_params=pltpu.CompilerParams(vmem_limit_bytes=VMEM_LIMIT),
    )(*args)


def expert(sources, w_gate, w_up, w_down):
    width = sources[0].shape[1]
    hidden = w_gate.shape[2]
    total = sum(s.shape[0] for s in sources)
    dtypes = [WIDE] + [NARROW] * (len(sources) - 1)
    vmem = pl.BlockSpec(memory_space=pltpu.VMEM)
    return pl.pallas_call(
        expert_kernel,
        out_shape=[jax.ShapeDtypeStruct(s.shape, d) for s, d in zip(sources, dtypes)],
        in_specs=[vmem] * len(sources) + [pl.BlockSpec(memory_space=pl.ANY)] * 3,
        out_specs=[vmem] * len(sources),
        scratch_shapes=[
            pltpu.VMEM((total, width), NARROW),
            pltpu.VMEM((total, hidden), NARROW),
            pltpu.VMEM((hidden // TILE, width, TILE), NARROW),
            pltpu.VMEM((hidden // TILE, width, TILE), NARROW),
            pltpu.VMEM((hidden, width), NARROW),
            pltpu.SemaphoreType.DMA((2 * (hidden // TILE) + 1,)),
        ],
        cost_estimate=pl.CostEstimate(
            flops=6 * total * width * hidden,
            bytes_accessed=6 * width * hidden + 8 * total * width,
            transcendentals=total * hidden,
        ),
        compiler_params=pltpu.CompilerParams(vmem_limit_bytes=VMEM_LIMIT),
    )(*sources, w_gate, w_up, w_down)


def gather_blocks(own):
    half = own.shape[0] // 2
    before = rotate(own, "tp", 1)
    after = rotate(own, "tp", -1)
    low, high = before[:half], after[half:]
    return [own, after, rotate(low, "tp", 1), rotate(high, "tp", -1), before]


def scatter_blocks(blocks):
    own, up, far_low, far_high, down = blocks
    half = own.shape[0] // 2
    from_before = rotate(far_low, "tp", 1)
    from_after = rotate(far_high, "tp", -1)
    up = jnp.concatenate(
        [(up[:half].astype(WIDE) + from_before.astype(WIDE)).astype(NARROW), up[half:]], axis=0
    )
    down = jnp.concatenate(
        [down[:half], (down[half:].astype(WIDE) + from_after.astype(WIDE)).astype(NARROW)],
        axis=0,
    )
    up = rotate(up, "tp", 1)
    down = rotate(down, "tp", -1)
    return [
        (own[p] + up[p].astype(WIDE) + down[p].astype(WIDE)).astype(NARROW)
        for p in (slice(0, half), slice(half, None))
    ]


def local(tokens, gain_in, routes, gates, w_gate, w_up, w_down, gain_out):
    count, width = tokens.shape
    choose = routes.shape[1]
    experts = lax.axis_size("ep")
    groups = lax.axis_size("tp")
    chips = experts // 2
    capacity = (3 * count * choose + 2 * experts - 1) // (2 * experts)
    span = experts * capacity
    part = capacity // CHUNKS
    lanes = width // groups
    rows = chips * 2 * part * groups
    block = chips * 2 * part
    me = lax.axis_index("tp")
    core = lax.axis_index("ep") % 2

    own_routes = lax.dynamic_slice_in_dim(routes, me * count, count, 0)
    own_gates = lax.dynamic_slice_in_dim(gates, me * count, count, 0)
    other_routes = partner(own_routes)
    other_tokens = partner(tokens)

    row = jnp.arange(rows, dtype=jnp.int32)[:, None]
    quarter = row % groups
    slot = (row // groups) % part
    side = (row // (groups * part)) % 2
    chip = row // (groups * part * 2)
    row_key = (quarter * 2 + side) * span + (2 * chip + core) * capacity + slot
    column_key = (quarter * span + (2 * chip + (core ^ side)) * capacity + slot).reshape(1, rows)
    back = quarter * block + (side * chips + chip) * part + slot
    line = jnp.arange(block, dtype=jnp.int32)[:, None]
    line_row = ((line // part) % chips * 2 + line // (part * chips)) * part + line % part
    line_row = line_row * groups
    quarters = (me + jnp.arange(groups, dtype=jnp.int32)) % groups * span

    outgoing = call(
        pack_kernel,
        [((rows, lanes), NARROW)] * CHUNKS,
        tokens,
        other_tokens,
        gain_in[None],
        own_routes,
        other_routes,
        row_key,
        capacity=capacity,
        span=span,
        groups=groups,
        flops=2 * CHUNKS * rows * 2 * count * width,
        moved=4 * count * width,
    )
    arrived = []
    for k in range(CHUNKS):
        arrived.append(exchange(outgoing[k].reshape(chips, -1, lanes)).reshape(rows, lanes))
    gains = [gain_out[None]]
    gains += [rotate(gain_out[None], "tp", -step) for step in range(1, groups)]

    returned = []
    for k in range(CHUNKS):
        (own,) = call(
            spread_kernel,
            [((block, width), NARROW)],
            arrived[k],
            line_row,
            groups=groups,
            flops=2 * block * rows * width,
            moved=4 * block * width,
        )
        sources = gather_blocks(own)
        parts = expert(sources, w_gate, w_up, w_down)
        kept, sent = scatter_blocks(parts)
        got = partner(sent)
        (leaving,) = call(
            leave_kernel,
            [((rows, lanes), NARROW)],
            kept,
            got,
            back,
            groups=groups,
            flops=2 * rows * block * width,
            moved=4 * block * width,
        )
        returned.append(exchange(leaving.reshape(chips, -1, lanes)).reshape(rows, lanes))

    final = call(
        finish_kernel,
        [((count, lanes), NARROW)] * groups,
        *returned,
        own_routes,
        other_routes,
        own_gates,
        column_key,
        quarters,
        *gains,
        smem=(CHUNKS + 4,),
        capacity=capacity,
        span=span,
        groups=groups,
        flops=4 * CHUNKS * rows * groups * count * lanes,
        moved=4 * rows * lanes,
    )
    final = [final[0]] + [rotate(final[step], "tp", step) for step in range(1, groups)]
    out = []
    for j in range(groups):
        piece = final[0]
        for step in range(1, groups):
            piece = jnp.where((me - step) % groups == j, final[step], piece)
        out.append(piece)
    return jnp.concatenate(out, axis=0)


def solution(mesh):
    in_specs = (
        P(("grp", "ep", "tp"), None),
        P(),
        P(("grp", "ep"), None),
        P(("grp", "ep"), None),
        P("ep", None, "tp"),
        P("ep", None, "tp"),
        P("ep", "tp", None),
        P("tp"),
    )
    out_specs = P(("grp", "ep"), "tp")
    return jax.shard_map(local, mesh=mesh, in_specs=in_specs, out_specs=out_specs, check_vma=False)
```

```python
import functools

import jax
import jax.numpy as jnp
from jax import lax
from jax.experimental import pallas as pl
from jax.experimental.pallas import tpu as pltpu
from jax.sharding import PartitionSpec as P


EPS = 1e-06
CHUNKS = 2
TILE = 256
OUT_TILE = 512
NARROW = jnp.bfloat16
WIDE = jnp.float32
VMEM_LIMIT = 48 * 1024 * 1024


def rotate(value, axis, step):
    size = lax.axis_size(axis)
    return lax.ppermute(value, axis, [(i, (i + step) % size) for i in range(size)])


def partner(value):
    return lax.ppermute(value, "ep", [(i, i ^ 1) for i in range(lax.axis_size("ep"))])


def exchange(value):
    size = lax.axis_size("ep")
    same = [list(range(core, size, 2)) for core in range(2)]
    return lax.all_to_all(value, "ep", 0, 0, tiled=True, axis_index_groups=same)


def dot(a, b):
    return jnp.dot(a, b, preferred_element_type=WIDE)


def one_hot(matches):
    return jnp.where(matches, 1.0, 0.0).astype(NARROW)


def places(own, other, capacity, span):
    both = jnp.concatenate([own * capacity, other * capacity + span], axis=0)
    column = jnp.concatenate([both[:, c : c + 1] for c in range(both.shape[1])], axis=0)
    total = column.shape[0]
    i = lax.broadcasted_iota(jnp.int32, (total, total), 0)
    j = lax.broadcasted_iota(jnp.int32, (total, total), 1)
    row = jnp.sum(jnp.where(i == j, column, 0), axis=0, keepdims=True)
    same = column == row
    row_slot = jnp.sum(jnp.where(same & (i < j), 1, 0), axis=0, keepdims=True)
    column_slot = jnp.sum(jnp.where(same & (j < i), 1, 0), axis=1, keepdims=True)
    return column + column_slot, row + row_slot


def pack_kernel(own, other, gain, own_routes, other_routes, row_key, *outs, capacity, span, groups):
    values = jnp.concatenate([own[...], other[...]], axis=0).astype(WIDE)
    scale = lax.rsqrt(jnp.mean(values * values, axis=-1, keepdims=True) + EPS)
    normed = (values * scale * gain[...]).astype(NARROW)
    _, row = places(own_routes[...], other_routes[...], capacity, span)
    rows = values.shape[0]
    lanes = values.shape[1] // groups
    for k, out in enumerate(outs):
        key = row_key[...] + k * (capacity // len(outs))
        total = None
        for q in range(groups):
            hit = key == row[:, :rows] + q * 2 * span
            for c in range(1, row.shape[1] // rows):
                hit = hit | (key == row[:, c * rows : (c + 1) * rows] + q * 2 * span)
            piece = dot(one_hot(hit), normed[:, q * lanes : (q + 1) * lanes])
            total = piece if total is None else total + piece
        out[...] = total.astype(NARROW)


def spread_kernel(arrived, line_row, out, *, groups):
    lanes = arrived.shape[1]
    column = lax.broadcasted_iota(jnp.int32, (line_row.shape[0], arrived.shape[0]), 1)
    for q in range(groups):
        pick = one_hot(line_row[...] + q == column)
        out[:, q * lanes : (q + 1) * lanes] = dot(pick, arrived[...]).astype(NARROW)


def expert_kernel(*refs):
    flat, hidden, wg, wu, wd, sems = refs[-6:]
    sinks, weights, sources = refs[-13:-6], refs[-16:-13], refs[:-16]
    steps = hidden.shape[1] // TILE
    loads = []
    for j in range(steps):
        part = pl.ds(j * TILE, TILE)
        for n, (source, kept) in enumerate(zip(weights, (wg, wu))):
            loads.append(
                pltpu.make_async_copy(source.at[0, :, part], kept.at[j], sems.at[2 * j + n])
            )
    loads.append(pltpu.make_async_copy(weights[2].at[0], wd, sems.at[2 * steps]))
    for load in loads:
        load.start()
    at = 0
    for source in sources:
        flat[at : at + source.shape[0], :] = source[...]
        at += source.shape[0]
    for j in range(steps):
        loads[2 * j].wait()
        loads[2 * j + 1].wait()
        gate = dot(flat[...], wg[j])
        up = dot(flat[...], wu[j])
        hidden[:, j * TILE : (j + 1) * TILE] = (gate / (1.0 + jnp.exp(-gate)) * up).astype(NARROW)
    loads[2 * steps].wait()

    def column(j, carry):
        lanes = pl.ds(pl.multiple_of(j * OUT_TILE, OUT_TILE), OUT_TILE)
        down = dot(hidden[...], wd[:, lanes])
        at = 0
        for sink in sinks:
            sink[:, lanes] = down[at : at + sink.shape[0], :].astype(sink.dtype)
            at += sink.shape[0]
        return carry

    lax.fori_loop(0, flat.shape[1] // OUT_TILE, column, 0)


def leave_kernel(kept, got, back, out, *, groups):
    both = jnp.concatenate([kept[...], got[...]], axis=0)
    lanes = both.shape[1] // groups
    column = lax.broadcasted_iota(jnp.int32, (out.shape[0], both.shape[0]), 1)
    total = None
    for q in range(groups):
        pick = one_hot(back[...] == column + q * both.shape[0])
        piece = dot(pick, both[:, q * lanes : (q + 1) * lanes])
        total = piece if total is None else total + piece
    out[...] = total.astype(NARROW)


def finish_kernel(*refs, capacity, span, groups):
    returned = refs[:CHUNKS]
    own_routes, other_routes, gates, column_key, quarters = refs[CHUNKS : CHUNKS + 5]
    gains = refs[CHUNKS + 5 : CHUNKS + 5 + groups]
    outs = refs[CHUNKS + 5 + groups :]
    column, _ = places(own_routes[...], other_routes[...], capacity, span)
    count, choose = gates.shape
    width = groups * returned[0].shape[1]
    total = None
    for k in range(CHUNKS):
        key = column_key[...] + k * (capacity // CHUNKS)
        blocks = []
        for step in range(groups):
            weight = 0.0
            for c in range(choose):
                place = column[2 * c * count : (2 * c + 1) * count, :] + quarters[step]
                weight = weight + jnp.where(place == key, gates[:, c : c + 1], 0.0)
            blocks.append(weight)
        weight = jnp.concatenate(blocks, axis=0)
        high = weight.astype(NARROW)
        low = (weight - high.astype(WIDE)).astype(NARROW)
        piece = dot(high, returned[k][...]) + dot(low, returned[k][...])
        total = piece if total is None else total + piece
    squares = 0.0
    for step in range(groups):
        block = total[step * count : (step + 1) * count, :]
        squares = squares + jnp.sum(block * block, axis=1, keepdims=True)
    scale = lax.rsqrt(squares / width + EPS)
    for step in range(groups):
        block = total[step * count : (step + 1) * count, :]
        outs[step][...] = (block * scale * gains[step][...]).astype(NARROW)


def whole(spec):
    return jax.ShapeDtypeStruct(spec[0], spec[1])


def call(kernel, outs, *args, flops=0, moved=0, smem=(), **kwargs):
    return pl.pallas_call(
        functools.partial(kernel, **kwargs),
        out_shape=[whole(o) for o in outs],
        in_specs=[
            pl.BlockSpec(memory_space=pltpu.SMEM if i in smem else pltpu.VMEM)
            for i in range(len(args))
        ],
        out_specs=[pl.BlockSpec(memory_space=pltpu.VMEM) for _ in outs],
        cost_estimate=pl.CostEstimate(flops=flops, bytes_accessed=moved, transcendentals=0),
        compiler_params=pltpu.CompilerParams(vmem_limit_bytes=VMEM_LIMIT),
    )(*args)


def expert(sources, w_gate, w_up, w_down):
    width = sources[0].shape[1]
    hidden = w_gate.shape[2]
    total = sum(s.shape[0] for s in sources)
    block = sources[0].shape[0]
    outs = [jax.ShapeDtypeStruct((block, width), WIDE)]
    outs += [jax.ShapeDtypeStruct((block // 2, width), NARROW)] * 6
    vmem = pl.BlockSpec(memory_space=pltpu.VMEM)
    return pl.pallas_call(
        expert_kernel,
        out_shape=outs,
        in_specs=[vmem] * len(sources) + [pl.BlockSpec(memory_space=pl.ANY)] * 3,
        out_specs=[vmem] * len(outs),
        scratch_shapes=[
            pltpu.VMEM((total, width), NARROW),
            pltpu.VMEM((total, hidden), NARROW),
            pltpu.VMEM((hidden // TILE, width, TILE), NARROW),
            pltpu.VMEM((hidden // TILE, width, TILE), NARROW),
            pltpu.VMEM((hidden, width), NARROW),
            pltpu.SemaphoreType.DMA((2 * (hidden // TILE) + 1,)),
        ],
        cost_estimate=pl.CostEstimate(
            flops=6 * total * width * hidden,
            bytes_accessed=6 * width * hidden + 8 * total * width,
            transcendentals=total * hidden,
        ),
        compiler_params=pltpu.CompilerParams(vmem_limit_bytes=VMEM_LIMIT),
    )(*sources, w_gate, w_up, w_down)


def gather_blocks(own):
    half = own.shape[0] // 2
    before = rotate(own, "tp", 1)
    after = rotate(own, "tp", -1)
    low, high = before[:half], after[half:]
    return [own, after, rotate(low, "tp", 1), rotate(high, "tp", -1), before]


def scatter_blocks(blocks):
    own, up_low, up_high, far_low, far_high, down_low, down_high = blocks
    half = own.shape[0] // 2

    def add(a, b):
        return (a.astype(WIDE) + b.astype(WIDE)).astype(NARROW)

    from_before = rotate(far_low, "tp", 1)
    from_after = rotate(far_high, "tp", -1)
    up_high = rotate(up_high, "tp", 1)
    down_low = rotate(down_low, "tp", -1)
    up_low = add(up_low, from_before)
    down_high = add(down_high, from_after)
    up_low = rotate(up_low, "tp", 1)
    down_high = rotate(down_high, "tp", -1)
    return [
        (own[:half] + up_low.astype(WIDE) + down_low.astype(WIDE)).astype(NARROW),
        (own[half:] + up_high.astype(WIDE) + down_high.astype(WIDE)).astype(NARROW),
    ]


def local(tokens, gain_in, routes, gates, w_gate, w_up, w_down, gain_out):
    count, width = tokens.shape
    choose = routes.shape[1]
    experts = lax.axis_size("ep")
    groups = lax.axis_size("tp")
    chips = experts // 2
    capacity = (3 * count * choose + 2 * experts - 1) // (2 * experts)
    span = experts * capacity
    part = capacity // CHUNKS
    lanes = width // groups
    rows = chips * 2 * part * groups
    block = chips * 2 * part
    me = lax.axis_index("tp")
    core = lax.axis_index("ep") % 2

    own_routes = lax.dynamic_slice_in_dim(routes, me * count, count, 0)
    own_gates = lax.dynamic_slice_in_dim(gates, me * count, count, 0)
    other_routes = partner(own_routes)
    other_tokens = partner(tokens)

    row = jnp.arange(rows, dtype=jnp.int32)[:, None]
    quarter = row % groups
    slot = (row // groups) % part
    side = (row // (groups * part)) % 2
    chip = row // (groups * part * 2)
    row_key = (quarter * 2 + side) * span + (2 * chip + core) * capacity + slot
    column_key = (quarter * span + (2 * chip + (core ^ side)) * capacity + slot).reshape(1, rows)
    back = quarter * block + (side * chips + chip) * part + slot
    line = jnp.arange(block, dtype=jnp.int32)[:, None]
    line_row = ((line // part) % chips * 2 + line // (part * chips)) * part + line % part
    line_row = line_row * groups
    quarters = (me + jnp.arange(groups, dtype=jnp.int32)) % groups * span

    outgoing = call(
        pack_kernel,
        [((rows, lanes), NARROW)] * CHUNKS,
        tokens,
        other_tokens,
        gain_in[None],
        own_routes,
        other_routes,
        row_key,
        capacity=capacity,
        span=span,
        groups=groups,
        flops=2 * CHUNKS * rows * 2 * count * width,
        moved=4 * count * width,
    )
    arrived = []
    for k in range(CHUNKS):
        arrived.append(exchange(outgoing[k].reshape(chips, -1, lanes)).reshape(rows, lanes))
    gains = [gain_out[None]]
    gains += [rotate(gain_out[None], "tp", -step) for step in range(1, groups)]

    returned = []
    for k in range(CHUNKS):
        (own,) = call(
            spread_kernel,
            [((block, width), NARROW)],
            arrived[k],
            line_row,
            groups=groups,
            flops=2 * block * rows * width,
            moved=4 * block * width,
        )
        sources = gather_blocks(own)
        parts = expert(sources, w_gate, w_up, w_down)
        kept, sent = scatter_blocks(parts)
        got = partner(sent)
        (leaving,) = call(
            leave_kernel,
            [((rows, lanes), NARROW)],
            kept,
            got,
            back,
            groups=groups,
            flops=2 * rows * block * width,
            moved=4 * block * width,
        )
        returned.append(exchange(leaving.reshape(chips, -1, lanes)).reshape(rows, lanes))

    final = call(
        finish_kernel,
        [((count, lanes), NARROW)] * groups,
        *returned,
        own_routes,
        other_routes,
        own_gates,
        column_key,
        quarters,
        *gains,
        smem=(CHUNKS + 4,),
        capacity=capacity,
        span=span,
        groups=groups,
        flops=4 * CHUNKS * rows * groups * count * lanes,
        moved=4 * rows * lanes,
    )
    kept = [final[0]]
    for step in range(1, groups):
        kept.append(rotate(final[step], "tp", step))
    final = kept
    out = []
    for j in range(groups):
        piece = final[0]
        for step in range(1, groups):
            piece = jnp.where((me - step) % groups == j, final[step], piece)
        out.append(piece)
    return jnp.concatenate(out, axis=0)


def solution(mesh):
    in_specs = (
        P(("grp", "ep", "tp"), None),
        P(),
        P(("grp", "ep"), None),
        P(("grp", "ep"), None),
        P("ep", None, "tp"),
        P("ep", None, "tp"),
        P("ep", "tp", None),
        P("tp"),
    )
    out_specs = P(("grp", "ep"), "tp")
    return jax.shard_map(local, mesh=mesh, in_specs=in_specs, out_specs=out_specs, check_vma=False)
```

```python
import functools

import jax
import jax.numpy as jnp
from jax import lax
from jax.experimental import pallas as pl
from jax.experimental.pallas import tpu as pltpu
from jax.sharding import PartitionSpec as P


EPS = 1e-06
CHUNKS = 2
TILE = 256
OUT_TILE = 1024
NARROW = jnp.bfloat16
WIDE = jnp.float32
VMEM_LIMIT = 48 * 1024 * 1024


def rotate(value, axis, step):
    size = lax.axis_size(axis)
    return lax.ppermute(value, axis, [(i, (i + step) % size) for i in range(size)])


def partner(value):
    return lax.ppermute(value, "ep", [(i, i ^ 1) for i in range(lax.axis_size("ep"))])


def exchange(value):
    size = lax.axis_size("ep")
    same = [list(range(core, size, 2)) for core in range(2)]
    return lax.all_to_all(value, "ep", 0, 0, tiled=True, axis_index_groups=same)


def dot(a, b):
    return jnp.dot(a, b, preferred_element_type=WIDE)


def one_hot(matches):
    return jnp.where(matches, 1.0, 0.0).astype(NARROW)


def places(own, other, capacity, span):
    both = jnp.concatenate([own * capacity, other * capacity + span], axis=0)
    column = jnp.concatenate([both[:, c : c + 1] for c in range(both.shape[1])], axis=0)
    total = column.shape[0]
    i = lax.broadcasted_iota(jnp.int32, (total, total), 0)
    j = lax.broadcasted_iota(jnp.int32, (total, total), 1)
    row = jnp.sum(jnp.where(i == j, column, 0), axis=0, keepdims=True)
    same = column == row
    row_slot = jnp.sum(jnp.where(same & (i < j), 1, 0), axis=0, keepdims=True)
    column_slot = jnp.sum(jnp.where(same & (j < i), 1, 0), axis=1, keepdims=True)
    return column + column_slot, row + row_slot


def pack_kernel(own, other, gain, own_routes, other_routes, row_key, *outs, capacity, span, groups):
    values = jnp.concatenate([own[...], other[...]], axis=0).astype(WIDE)
    scale = lax.rsqrt(jnp.mean(values * values, axis=-1, keepdims=True) + EPS)
    normed = (values * scale * gain[...]).astype(NARROW)
    _, row = places(own_routes[...], other_routes[...], capacity, span)
    rows = values.shape[0]
    lanes = values.shape[1] // groups
    for k, out in enumerate(outs):
        key = row_key[...] + k * (capacity // len(outs))
        total = None
        for q in range(groups):
            hit = key == row[:, :rows] + q * 2 * span
            for c in range(1, row.shape[1] // rows):
                hit = hit | (key == row[:, c * rows : (c + 1) * rows] + q * 2 * span)
            piece = dot(one_hot(hit), normed[:, q * lanes : (q + 1) * lanes])
            total = piece if total is None else total + piece
        out[...] = total.astype(NARROW)


def spread_kernel(arrived, line_row, out, *, groups):
    lanes = arrived.shape[1]
    column = lax.broadcasted_iota(jnp.int32, (line_row.shape[0], arrived.shape[0]), 1)
    for q in range(groups):
        pick = one_hot(line_row[...] + q == column)
        out[:, q * lanes : (q + 1) * lanes] = dot(pick, arrived[...]).astype(NARROW)


def expert_kernel(*refs):
    flat, hidden, wg, wu, wd, sems = refs[-6:]
    sinks, weights, sources = refs[-13:-6], refs[-16:-13], refs[:-16]
    steps = hidden.shape[1] // TILE
    loads = []
    for j in range(steps):
        part = pl.ds(j * TILE, TILE)
        for n, (source, kept) in enumerate(zip(weights, (wg, wu))):
            loads.append(
                pltpu.make_async_copy(source.at[0, :, part], kept.at[j], sems.at[2 * j + n])
            )
    loads.append(pltpu.make_async_copy(weights[2].at[0], wd, sems.at[2 * steps]))
    for load in loads:
        load.start()
    at = 0
    for source in sources:
        flat[at : at + source.shape[0], :] = source[...]
        at += source.shape[0]
    for j in range(steps):
        loads[2 * j].wait()
        loads[2 * j + 1].wait()
        gate = dot(flat[...], wg[j])
        up = dot(flat[...], wu[j])
        hidden[:, j * TILE : (j + 1) * TILE] = (gate / (1.0 + jnp.exp(-gate)) * up).astype(NARROW)
    loads[2 * steps].wait()
    for j in range(0, flat.shape[1], OUT_TILE):
        lanes = pl.ds(j, OUT_TILE)
        down = dot(hidden[...], wd[:, lanes])
        at = 0
        for sink in sinks:
            sink[:, lanes] = down[at : at + sink.shape[0], :].astype(sink.dtype)
            at += sink.shape[0]


def leave_kernel(kept, got, back, out, *, groups):
    both = jnp.concatenate([kept[...], got[...]], axis=0)
    lanes = both.shape[1] // groups
    column = lax.broadcasted_iota(jnp.int32, (out.shape[0], both.shape[0]), 1)
    total = None
    for q in range(groups):
        pick = one_hot(back[...] == column + q * both.shape[0])
        piece = dot(pick, both[:, q * lanes : (q + 1) * lanes])
        total = piece if total is None else total + piece
    out[...] = total.astype(NARROW)


def finish_kernel(*refs, capacity, span, groups):
    returned = refs[:CHUNKS]
    own_routes, other_routes, gates, column_key, quarters = refs[CHUNKS : CHUNKS + 5]
    outs = refs[CHUNKS + 5 :]
    column, _ = places(own_routes[...], other_routes[...], capacity, span)
    count, choose = gates.shape
    width = groups * returned[0].shape[1]
    total = None
    for k in range(CHUNKS):
        key = column_key[...] + k * (capacity // CHUNKS)
        blocks = []
        for step in range(groups):
            weight = 0.0
            for c in range(choose):
                place = column[2 * c * count : (2 * c + 1) * count, :] + quarters[step]
                weight = weight + jnp.where(place == key, gates[:, c : c + 1], 0.0)
            blocks.append(weight)
        weight = jnp.concatenate(blocks, axis=0)
        high = weight.astype(NARROW)
        low = (weight - high.astype(WIDE)).astype(NARROW)
        piece = dot(high, returned[k][...]) + dot(low, returned[k][...])
        total = piece if total is None else total + piece
    squares = 0.0
    for step in range(groups):
        block = total[step * count : (step + 1) * count, :]
        squares = squares + jnp.sum(block * block, axis=1, keepdims=True)
    scale = lax.rsqrt(squares / width + EPS)
    for step in range(groups):
        block = total[step * count : (step + 1) * count, :]
        outs[step][...] = (block * scale).astype(NARROW)


def whole(spec):
    return jax.ShapeDtypeStruct(spec[0], spec[1])


def call(kernel, outs, *args, flops=0, moved=0, smem=(), **kwargs):
    return pl.pallas_call(
        functools.partial(kernel, **kwargs),
        out_shape=[whole(o) for o in outs],
        in_specs=[
            pl.BlockSpec(memory_space=pltpu.SMEM if i in smem else pltpu.VMEM)
            for i in range(len(args))
        ],
        out_specs=[pl.BlockSpec(memory_space=pltpu.VMEM) for _ in outs],
        cost_estimate=pl.CostEstimate(flops=flops, bytes_accessed=moved, transcendentals=0),
        compiler_params=pltpu.CompilerParams(vmem_limit_bytes=VMEM_LIMIT),
    )(*args)


def expert(sources, w_gate, w_up, w_down):
    width = sources[0].shape[1]
    hidden = w_gate.shape[2]
    total = sum(s.shape[0] for s in sources)
    block = sources[0].shape[0]
    outs = [jax.ShapeDtypeStruct((block, width), WIDE)]
    outs += [jax.ShapeDtypeStruct((block // 2, width), NARROW)] * 6
    vmem = pl.BlockSpec(memory_space=pltpu.VMEM)
    return pl.pallas_call(
        expert_kernel,
        out_shape=outs,
        in_specs=[vmem] * len(sources) + [pl.BlockSpec(memory_space=pl.ANY)] * 3,
        out_specs=[vmem] * len(outs),
        scratch_shapes=[
            pltpu.VMEM((total, width), NARROW),
            pltpu.VMEM((total, hidden), NARROW),
            pltpu.VMEM((hidden // TILE, width, TILE), NARROW),
            pltpu.VMEM((hidden // TILE, width, TILE), NARROW),
            pltpu.VMEM((hidden, width), NARROW),
            pltpu.SemaphoreType.DMA((2 * (hidden // TILE) + 1,)),
        ],
        cost_estimate=pl.CostEstimate(
            flops=6 * total * width * hidden,
            bytes_accessed=6 * width * hidden + 8 * total * width,
            transcendentals=total * hidden,
        ),
        compiler_params=pltpu.CompilerParams(vmem_limit_bytes=VMEM_LIMIT),
    )(*sources, w_gate, w_up, w_down)


def gather_blocks(own, k):
    half = own.shape[0] // 2
    if k == CHUNKS - 1:
        low, high = own[:half], own[half:]
        before_low = rotate(low, "tp", 1)
        after_high = rotate(high, "tp", -1)
        before_high = rotate(high, "tp", 1)
        after_low = rotate(low, "tp", -1)
        far = [rotate(before_low, "tp", 1), rotate(after_high, "tp", -1)]
        return [own, after_low, after_high, *far, before_low, before_high]
    before = rotate(own, "tp", 1)
    after = rotate(own, "tp", -1)
    low, high = before[:half], after[half:]
    return [own, after, rotate(low, "tp", 1), rotate(high, "tp", -1), before]


def scatter_blocks(blocks):
    own, up_low, up_high, far_low, far_high, down_low, down_high = blocks
    half = own.shape[0] // 2

    def add(a, b):
        return (a.astype(WIDE) + b.astype(WIDE)).astype(NARROW)

    from_before = rotate(far_low, "tp", 1)
    from_after = rotate(far_high, "tp", -1)
    up_high = rotate(up_high, "tp", 1)
    down_low = rotate(down_low, "tp", -1)
    up_low = add(up_low, from_before)
    down_high = add(down_high, from_after)
    up_low = rotate(up_low, "tp", 1)
    down_high = rotate(down_high, "tp", -1)
    return [
        (own[:half] + up_low.astype(WIDE) + down_low.astype(WIDE)).astype(NARROW),
        (own[half:] + up_high.astype(WIDE) + down_high.astype(WIDE)).astype(NARROW),
    ]


def local(tokens, gain_in, routes, gates, w_gate, w_up, w_down, gain_out):
    count, width = tokens.shape
    choose = routes.shape[1]
    experts = lax.axis_size("ep")
    groups = lax.axis_size("tp")
    chips = experts // 2
    capacity = (3 * count * choose + 2 * experts - 1) // (2 * experts)
    span = experts * capacity
    part = capacity // CHUNKS
    lanes = width // groups
    rows = chips * 2 * part * groups
    block = chips * 2 * part
    me = lax.axis_index("tp")
    core = lax.axis_index("ep") % 2

    own_routes = lax.dynamic_slice_in_dim(routes, me * count, count, 0)
    own_gates = lax.dynamic_slice_in_dim(gates, me * count, count, 0)
    other_routes = partner(own_routes)
    other_tokens = partner(tokens)

    row = jnp.arange(rows, dtype=jnp.int32)[:, None]
    quarter = row % groups
    slot = (row // groups) % part
    side = (row // (groups * part)) % 2
    chip = row // (groups * part * 2)
    row_key = (quarter * 2 + side) * span + (2 * chip + core) * capacity + slot
    column_key = (quarter * span + (2 * chip + (core ^ side)) * capacity + slot).reshape(1, rows)
    back = quarter * block + (side * chips + chip) * part + slot
    line = jnp.arange(block, dtype=jnp.int32)[:, None]
    line_row = ((line // part) % chips * 2 + line // (part * chips)) * part + line % part
    line_row = line_row * groups
    quarters = (me + jnp.arange(groups, dtype=jnp.int32)) % groups * span

    outgoing = call(
        pack_kernel,
        [((rows, lanes), NARROW)] * CHUNKS,
        tokens,
        other_tokens,
        gain_in[None],
        own_routes,
        other_routes,
        row_key,
        capacity=capacity,
        span=span,
        groups=groups,
        flops=2 * CHUNKS * rows * 2 * count * width,
        moved=4 * count * width,
    )
    arrived = []
    for k in range(CHUNKS):
        arrived.append(exchange(outgoing[k].reshape(chips, -1, lanes)).reshape(rows, lanes))
    returned = []
    for k in range(CHUNKS):
        (own,) = call(
            spread_kernel,
            [((block, width), NARROW)],
            arrived[k],
            line_row,
            groups=groups,
            flops=2 * block * rows * width,
            moved=4 * block * width,
        )
        sources = gather_blocks(own, k)
        parts = expert(sources, w_gate, w_up, w_down)
        kept, sent = scatter_blocks(parts)
        got = partner(sent)
        (leaving,) = call(
            leave_kernel,
            [((rows, lanes), NARROW)],
            kept,
            got,
            back,
            groups=groups,
            flops=2 * rows * block * width,
            moved=4 * block * width,
        )
        returned.append(exchange(leaving.reshape(chips, -1, lanes)).reshape(rows, lanes))

    final = call(
        finish_kernel,
        [((count, lanes), NARROW)] * groups,
        *returned,
        own_routes,
        other_routes,
        own_gates,
        column_key,
        quarters,
        smem=(CHUNKS + 4,),
        capacity=capacity,
        span=span,
        groups=groups,
        flops=4 * CHUNKS * rows * groups * count * lanes,
        moved=4 * rows * lanes,
    )
    kept = [final[0]]
    for step in range(1, groups):
        kept.append(rotate(final[step], "tp", step))
    final = kept
    out = []
    for j in range(groups):
        piece = final[0]
        for step in range(1, groups):
            piece = jnp.where((me - step) % groups == j, final[step], piece)
        out.append(piece)
    out = jnp.concatenate(out, axis=0).astype(WIDE)
    return (out * gain_out).astype(NARROW)


def solution(mesh):
    in_specs = (
        P(("grp", "ep", "tp"), None),
        P(),
        P(("grp", "ep"), None),
        P(("grp", "ep"), None),
        P("ep", None, "tp"),
        P("ep", None, "tp"),
        P("ep", "tp", None),
        P("tp"),
    )
    out_specs = P(("grp", "ep"), "tp")
    return jax.shard_map(local, mesh=mesh, in_specs=in_specs, out_specs=out_specs, check_vma=False)
```
